32 devices in a mesh: ep: 8 (over z, core), tp: 4 (over y, x).
Axes of the slice: x: 2, y: 2, z: 4, core: 2. Of those that a mesh axis runs over, the one named last changes fastest.
Arguments:
- receptance: bfloat16 [2048, 2048], P('ep', 'tp'), may hold values from -6 to 6
- key_tensor: bfloat16 [2048, 2048], P('ep', 'tp'), may hold values from -6 to 6
- value_tensor: bfloat16 [2048, 2048], P('ep', 'tp'), may hold values from -6 to 6
- decay_data_input: bfloat16 [2048, 2048], P('ep', 'tp'), may hold values from -4 to 4
- correction_rate_input: bfloat16 [2048, 2048], P('ep', 'tp'), may hold values from -16 to 6
- mixer_output_gate: bfloat16 [2048, 2048], P('ep', 'tp'), may hold values from -6 to 6
- decay_channel_offset: float32 [2048], P('tp'), may hold values from -16 to -3
- head_norm_gain: float32 [2048], P('tp'), may hold values from 0.1 to 1.9
- self_key_weight: float32 [2048], P('tp'), may hold values from -2 to 2
- mixer_output_weight: bfloat16 [2048, 2048], P('tp'), may hold values from -0.125 to 0.125
- second_batch_rows: bfloat16 [1024, 2048], P('ep'), may hold values from -6 to 6
- routed_expert_index: int32 [1024, 4], P('ep'), may hold values from 0 to 7, all different within a row; in each aligned block of 128 rows (0 to 127, 128 to 255, ...) at most 96 rows name the same one
- routing_output_weight: float32 [1024, 4], P('ep'), may hold values from 0.1 to 1
- expert_norm_gain: float32 [2048], replicated, may hold values from 0.1 to 1.9
- expert_gate_weight: bfloat16 [8, 1024, 2048], P('ep', 'tp'), may hold values from -0.125 to 0.125
- expert_up_weight: bfloat16 [8, 1024, 2048], P('ep', 'tp'), may hold values from -0.125 to 0.125
- expert_down_weight: bfloat16 [8, 1024, 2048], P('ep', None, 'tp'), may hold values from -0.1875 to 0.1875
- common_expert_gate: bfloat16 [1024, 2048], P('tp'), may hold values from -0.125 to 0.125
- common_expert_up: bfloat16 [1024, 2048], P('tp'), may hold values from -0.125 to 0.125
- common_expert_down: bfloat16 [1024, 2048], P(None, 'tp'), may hold values from -0.1875 to 0.1875
Outputs:
- token_mixer_output: bfloat16 [2048, 2048], P(('ep', 'tp'))
- expert_out: bfloat16 [1024, 2048], P('ep', 'tp')
The draws below stay inside these ranges and needn't reach their ends.
Inputs may be any that keep to these rules, and one draw needn't show every extreme that they name: `routed_expert_index`: each row names 4 different experts. Within the rows of one index of ep no expert is named by more than 96 rows, and that bound is met in some index's rows.
All inputs are finite; a program needn't handle non-finite values.
Results may differ from the reference program's by a relative error of at most 0.017.
Values may be sent and summed in bfloat16 or wider, within the bound.
No kernel may reach another device: no remote copies, remote signals or barrier semaphores. Data moves between devices by JAX's collectives and lax.ppermute only.
A program may use at most 128 MiB of HBM per device.

```python
import math
import jax
import jax.numpy as jnp
import numpy as np
from jax import lax

MODEL_WIDTH = 2048
HEADS = 32
HEAD_CHANNELS = 64
FF = 1024
TOP = 4
ROWS_EXP = 128
SEQ_MIX = 2048
TOKENS_EXP = 1024
EXPERTS = 8
CAP = 96
N_EP = 8
N_TP = 4


def slow_marks(key):
    picks = jax.random.randint(jax.random.fold_in(key, 7), (HEADS,), 0, 10)
    return picks < 5


def draw_decay_channel_offset(key, part):
    slow_heads = slow_marks(key)
    spread = jax.random.uniform(jax.random.fold_in(key, 11), (HEADS, HEAD_CHANNELS), jnp.float32)
    slow_base = jnp.log(0.4 / SEQ_MIX) + 0.5 - spread
    fast_base = -4.0 + spread
    return jnp.where(slow_heads[:, None], slow_base, fast_base).reshape(MODEL_WIDTH).astype(jnp.float32)


def draw_correction_rate_input(key, part):
    slow_heads = slow_marks(key)
    offset = jnp.where(slow_heads, jnp.log(0.3 * HEAD_CHANNELS / SEQ_MIX), 0.0)
    jitter = jnp.clip(jax.random.normal(jax.random.fold_in(key, 13), (SEQ_MIX, HEADS, HEAD_CHANNELS), jnp.float32), -6.0, 6.0)
    return (jitter + offset[None, :, None]).reshape(SEQ_MIX, MODEL_WIDTH).astype(jnp.bfloat16)


def draw_decay_data_input(key, part):
    blocks = SEQ_MIX // 64
    shifts = jax.random.uniform(jax.random.fold_in(key, 17), (blocks, 1, MODEL_WIDTH), jnp.float32, -1.0, 1.0)
    jitter = 0.6 * jnp.clip(jax.random.normal(jax.random.fold_in(key, 19), (blocks, 64, MODEL_WIDTH), jnp.float32), -5.0, 5.0)
    return (jitter + shifts).reshape(SEQ_MIX, MODEL_WIDTH).astype(jnp.bfloat16)


def level_of(own_key, shape, shards, least, top_value):
    loudness, own = 1.0, jax.random.fold_in(own_key, 6)
    for axis_at, blocks in shards:
        draws = jnp.exp(jax.random.uniform(jax.random.fold_in(own, axis_at), (blocks,), jnp.float32, least / len(shards), top_value / len(shards)))
        loudness = loudness * jnp.repeat(draws, shape[axis_at] // blocks).reshape([-1 if axis == axis_at else 1 for axis in range(len(shape))])
    return loudness


def deal_out(own_key, own, number, rows, count, top, reach, slope):
    order = jax.random.permutation(own_key, count)
    crowded, ordinary = portions_of(count, rows * top, reach, slope, True), portions_of(count, rows * top, reach, slope, False)
    places = jnp.arange(count)

    def named(lengths, rotation):
        used = int((lengths > 0).sum())
        fixed = max(1, used // 4)
        moved = fixed + (places - fixed + rotation * (used - fixed)) % max(1, count - fixed)
        return jnp.zeros((count,), jnp.int32).at[order[jnp.where(places < fixed, places, moved)]].set(jnp.asarray(lengths, jnp.int32))

    lengths = jnp.where(number % 4 == 0, named(crowded, number // 4), named(ordinary, number - number // 4 - 1))
    mixed = jax.random.permutation(jax.random.fold_in(own, 3), count)
    source_of, taker = mixed[0:count // 2 * 2:2], mixed[1:count // 2 * 2:2]
    slack = jnp.minimum(lengths[source_of] - 1, reach - lengths[taker]) // 2
    slack = jnp.where((source_of == order[0]) | (taker == order[0]) | (lengths[taker] == 0), 0, jnp.maximum(slack, 0))
    moved = jax.random.randint(jax.random.fold_in(own, 4), (count // 2,), 0, 1 << 20) % (slack + 1)
    lengths = lengths.at[source_of].add(-moved).at[taker].add(moved)
    labels = jnp.searchsorted(jnp.cumsum(lengths), jnp.arange(rows * top), side="right").astype(jnp.int32)
    grid = labels.reshape(top, rows).T
    grid = grid[jax.random.permutation(jax.random.fold_in(own, 1), rows)]
    rotation = jax.random.randint(jax.random.fold_in(own, 2), (rows, 1), 0, top)
    return jnp.take_along_axis(grid, (jnp.arange(top)[None, :] + rotation) % top, axis=1)


def portions_of(amount, total, bound, skew, full):
    loads = [(1 << 20) // math.isqrt(grade ** skew) + 1 for grade in range(1, amount + 1)]
    largest = bound if full else min(bound, max(-(-total // amount), total * loads[0] // sum(loads)))
    least = 1 if total - largest >= amount - 1 else 0
    given, rest = [largest] + [least] * (amount - 1), total - largest - least * (amount - 1)
    while rest > 0:
        candidates = [i for i in range(1, amount) if given[i] < largest] or [i for i in range(1, amount) if given[i] < bound]
        whole, budget = sum([loads[i] for i in candidates]), rest
        for i in candidates:
            extra = min(bound - given[i], max(1, budget * loads[i] // whole), rest)
            given[i] = given[i] + extra
            rest = rest - extra
    return np.array(given)


def noise(own_key, extent, deviation, bound, cuts=(), kind=jnp.bfloat16):
    gain = level_of(own_key, extent, cuts, -0.22, 0.18) if cuts else 1.0
    values = jax.random.normal(own_key, extent, jnp.float32) * deviation * gain
    return jnp.minimum(jnp.maximum(values, -bound), bound).astype(kind)


def setup_inputs(seed: int = 0) -> dict:
    keys = jax.random.split(jax.random.key(seed), 21)
    receptance = noise(keys[0], (SEQ_MIX, MODEL_WIDTH), 1.0, 6.0, ((0, 8), (1, 4)))
    key_tensor = noise(keys[1], (SEQ_MIX, MODEL_WIDTH), 1.0, 6.0, ((0, 8), (1, 4)))
    value_tensor = noise(keys[2], (SEQ_MIX, MODEL_WIDTH), 1.0, 6.0, ((0, 8), (1, 4)))
    decay_data_input = draw_decay_data_input(jax.random.fold_in(keys[20], 71), 0)
    correction_rate_input = draw_correction_rate_input(jax.random.fold_in(keys[20], 71), 0)
    mixer_output_gate = noise(keys[5], (SEQ_MIX, MODEL_WIDTH), 1.0, 6.0, ((0, 8), (1, 4)))
    decay_channel_offset = draw_decay_channel_offset(jax.random.fold_in(keys[20], 71), 0)
    head_norm_gain = jnp.clip(1.0 + 0.18 * jax.random.normal(keys[7], (MODEL_WIDTH,), jnp.float32), 0.1, 1.9)
    self_key_weight = noise(keys[8], (MODEL_WIDTH,), 0.15, 2.0, ((0, 4),), jnp.float32)
    mixer_output_weight = noise(keys[9], (MODEL_WIDTH, MODEL_WIDTH), MODEL_WIDTH ** -0.5, 0.125, ((0, 4),))
    second_batch_rows = noise(keys[10], (TOKENS_EXP, MODEL_WIDTH), 1.0, 6.0, ((0, 8),))
    routed_expert_index_keys = jax.random.split(jax.random.fold_in(keys[11], 1), TOKENS_EXP // ROWS_EXP)
    routed_expert_index_turns = jax.random.permutation(jax.random.fold_in(keys[11], 3), TOKENS_EXP // ROWS_EXP)
    routed_expert_index = jax.vmap(lambda own, number: deal_out(jax.random.fold_in(keys[11], 2), own, number, ROWS_EXP, EXPERTS, TOP, CAP, 1))(routed_expert_index_keys, routed_expert_index_turns).reshape((TOKENS_EXP, TOP))
    routing_output_weight = jnp.clip(0.1 + 0.9 * jax.random.uniform(keys[12], (TOKENS_EXP, TOP), jnp.float32) ** level_of(keys[12], (TOKENS_EXP, TOP), ((0, 8),), -0.2, 0.2), 0.1, 1.0)
    expert_norm_gain = jnp.clip(1.0 + 0.18 * jax.random.normal(keys[13], (MODEL_WIDTH,), jnp.float32), 0.1, 1.9)
    expert_gate_weight = noise(keys[14], (EXPERTS, FF, MODEL_WIDTH), MODEL_WIDTH ** -0.5, 0.125, ((0, 8), (1, 4)))
    expert_up_weight = noise(keys[15], (EXPERTS, FF, MODEL_WIDTH), MODEL_WIDTH ** -0.5, 0.125, ((0, 8), (1, 4)))
    expert_down_weight = noise(keys[16], (EXPERTS, FF, MODEL_WIDTH), FF ** -0.5, 0.1875, ((0, 8), (2, 4)))
    common_expert_gate = noise(keys[17], (FF, MODEL_WIDTH), MODEL_WIDTH ** -0.5, 0.125, ((0, 4),))
    common_expert_up = noise(keys[18], (FF, MODEL_WIDTH), MODEL_WIDTH ** -0.5, 0.125, ((0, 4),))
    common_expert_down = noise(keys[19], (FF, MODEL_WIDTH), FF ** -0.5, 0.1875, ((1, 4),))
    return dict(receptance=receptance, key_tensor=key_tensor, value_tensor=value_tensor, decay_data_input=decay_data_input, correction_rate_input=correction_rate_input, mixer_output_gate=mixer_output_gate, decay_channel_offset=decay_channel_offset, head_norm_gain=head_norm_gain, self_key_weight=self_key_weight, mixer_output_weight=mixer_output_weight, second_batch_rows=second_batch_rows, routed_expert_index=routed_expert_index, routing_output_weight=routing_output_weight, expert_norm_gain=expert_norm_gain, expert_gate_weight=expert_gate_weight, expert_up_weight=expert_up_weight, expert_down_weight=expert_down_weight, common_expert_gate=common_expert_gate, common_expert_up=common_expert_up, common_expert_down=common_expert_down)


HIGHEST = lax.Precision.HIGHEST
NORM_FLOOR = 1.0

def decay_terms(decay_data_input, correction_rate_input, decay_channel_offset):
    pre_log = -jax.nn.softplus(-(decay_channel_offset + decay_data_input.astype(jnp.float32))) - 0.5
    return (jnp.exp(-jnp.exp(pre_log)), jax.nn.sigmoid(correction_rate_input.astype(jnp.float32)))

def head_view(matrix):
    return matrix.astype(jnp.float32).reshape(matrix.shape[0], -1, HEAD_CHANNELS)

def complete_head_outputs(state_readout, receptance_rows, key_row_block, value_row_block, head_norm_gain, self_key_weight, mixer_output_gate):
    mean_part = lax.optimization_barrier(jnp.mean(state_readout, axis=-1, keepdims=True))
    spread = lax.optimization_barrier(jnp.mean(jnp.square(state_readout - mean_part), axis=-1, keepdims=True))
    normalized_rows = (state_readout - mean_part) * lax.rsqrt(spread + NORM_FLOOR)
    sequence_length = state_readout.shape[0]
    normalized_rows = normalized_rows.reshape(sequence_length, -1) * head_norm_gain
    self_key_term = lax.optimization_barrier(jnp.sum(receptance_rows * key_row_block * self_key_weight.reshape(-1, HEAD_CHANNELS), axis=-1, keepdims=True)) * value_row_block
    mixer_result = (normalized_rows + self_key_term.reshape(sequence_length, -1)) * mixer_output_gate.astype(jnp.float32)
    return mixer_result.astype(jnp.bfloat16)

def token_mixer_baseline(receptance, key_tensor, value_tensor, decay_data_input, correction_rate_input, mixer_output_gate, decay_channel_offset, head_norm_gain, self_key_weight, mixer_output_weight):
    decays, rates = decay_terms(decay_data_input, correction_rate_input, decay_channel_offset)
    receptance_rows = head_view(receptance)
    key_row_block = head_view(key_tensor)
    value_row_block = head_view(value_tensor)
    unit_keys = key_row_block * lax.rsqrt(lax.optimization_barrier(jnp.sum(key_row_block * key_row_block, axis=-1, keepdims=True)) + 1.0)
    decays = decays.reshape(key_row_block.shape)
    rates = rates.reshape(key_row_block.shape)

    def advance(memory, inputs):
        recept_now, decay_now, key_now, value_now, unit_now, rate_now = inputs
        projected = jnp.einsum('hij,hj->hi', memory, unit_now, precision=HIGHEST)
        memory = memory * decay_now[:, None, :] - projected[:, :, None] * (unit_now * rate_now)[:, None, :] + value_now[:, :, None] * key_now[:, None, :]
        return (memory, jnp.einsum('hij,hj->hi', memory, recept_now, precision=HIGHEST))
    head_count = key_row_block.shape[1]
    initial = jnp.zeros((head_count, HEAD_CHANNELS, HEAD_CHANNELS), jnp.float32)
    _, state_readout = lax.scan(advance, initial, (receptance_rows, decays, key_row_block, value_row_block, unit_keys, rates))
    mixer_result = complete_head_outputs(state_readout, receptance_rows, key_row_block, value_row_block, head_norm_gain, self_key_weight, mixer_output_gate)
    groups = mixer_result.reshape(SEQ_MIX, N_TP, MODEL_WIDTH // N_TP).transpose(1, 0, 2)
    weights = mixer_output_weight.reshape(N_TP, MODEL_WIDTH // N_TP, MODEL_WIDTH)

    def add_group(running, blocks):
        mixed_part, weight_part = blocks
        partial_sum = jnp.dot(mixed_part, weight_part, preferred_element_type=jnp.float32).astype(jnp.bfloat16)
        partial_sum = lax.optimization_barrier(partial_sum)
        return (running + partial_sum.astype(jnp.float32), None)
    summed, _ = lax.scan(add_group, jnp.zeros((SEQ_MIX, MODEL_WIDTH), jnp.float32), (groups, weights))
    return summed.astype(jnp.bfloat16)

def expert_unit(rows_in, gate_part, up_part, down_part):
    pre_gate = jnp.dot(rows_in, gate_part.T, preferred_element_type=jnp.float32)
    pre_up = jnp.dot(rows_in, up_part.T, preferred_element_type=jnp.float32)
    hidden = (jax.nn.silu(pre_gate) * pre_up).astype(jnp.bfloat16)
    return jnp.dot(hidden, down_part, preferred_element_type=jnp.float32)

def experts_reference(second_batch_rows, routed_expert_index, routing_output_weight, expert_norm_gain, expert_gate_weight, expert_up_weight, expert_down_weight, common_expert_gate, common_expert_up, common_expert_down):
    widened = second_batch_rows.astype(jnp.float32)
    normalized_rows = (widened * lax.rsqrt(lax.optimization_barrier(jnp.mean(widened * widened, axis=-1, keepdims=True)) + NORM_FLOOR) * expert_norm_gain).astype(jnp.bfloat16)
    shared_out = expert_unit(normalized_rows, common_expert_gate, common_expert_up, common_expert_down)
    flat_ids = routed_expert_index.reshape(-1).astype(jnp.int32)
    ordering = jnp.argsort(flat_ids, stable=True).astype(jnp.int32)
    counts = lax.optimization_barrier(jnp.sum((flat_ids[:, None] == jnp.arange(EXPERTS, dtype=jnp.int32)[None, :]).astype(jnp.int32), axis=0))
    firsts = (jnp.cumsum(counts) - counts).astype(jnp.int32)
    capacity = N_EP * CAP
    padded_order = jnp.concatenate([ordering, jnp.zeros((capacity,), jnp.int32)])
    flat_weights = routing_output_weight.reshape(-1)

    def visit(summed, expert):
        chosen = lax.dynamic_slice_in_dim(padded_order, firsts[expert], capacity)
        usable = jnp.arange(capacity) < counts[expert]
        tokens = chosen // TOP
        copies = expert_unit(normalized_rows[tokens], expert_gate_weight[expert], expert_up_weight[expert], expert_down_weight[expert]).astype(jnp.bfloat16)
        copies = lax.optimization_barrier(copies).astype(jnp.float32)
        factor = jnp.where(usable, flat_weights[chosen], 0.0)
        return (summed.at[tokens].add(copies * factor[:, None]), None)
    routed, _ = lax.scan(visit, jnp.zeros((TOKENS_EXP, MODEL_WIDTH), jnp.float32), jnp.arange(EXPERTS))
    return (routed + shared_out).astype(jnp.bfloat16)

def reference(receptance, key_tensor, value_tensor, decay_data_input, correction_rate_input, mixer_output_gate, decay_channel_offset, head_norm_gain, self_key_weight, mixer_output_weight, second_batch_rows, routed_expert_index, routing_output_weight, expert_norm_gain, expert_gate_weight, expert_up_weight, expert_down_weight, common_expert_gate, common_expert_up, common_expert_down):
    token_mixer_output = token_mixer_baseline(receptance, key_tensor, value_tensor, decay_data_input, correction_rate_input, mixer_output_gate, decay_channel_offset, head_norm_gain, self_key_weight, mixer_output_weight)
    expert_out = experts_reference(second_batch_rows, routed_expert_index, routing_output_weight, expert_norm_gain, expert_gate_weight, expert_up_weight, expert_down_weight, common_expert_gate, common_expert_up, common_expert_down)
    return (token_mixer_output, expert_out)
```

```python
import functools

import jax
import jax.numpy as jnp
from jax import lax
from jax.experimental import pallas as pl
from jax.experimental.pallas import tpu as pltpu
from jax.sharding import PartitionSpec as P

HEAD = 64
PAIR = 2 * HEAD
CHUNK = 64
NORM_FLOOR = 1.0
DECAY_SCALE = 0.6065306597126334
BF = jnp.bfloat16
F32 = jnp.float32
NN = (((1,), (0,)), ((), ()))
NT = (((1,), (1,)), ((), ()))
TN = (((0,), (0,)), ((), ()))


def dot1(a, b, dims=NN):
    return lax.dot_general(a.astype(BF), b.astype(BF), dims, preferred_element_type=F32)


def split(x):
    hi = x.astype(BF)
    return hi, (x - hi.astype(F32)).astype(BF)


def dot3(a, b, dims=NN):
    ah, al = split(a)
    bh, bl = split(b)
    d = functools.partial(lax.dot_general, dimension_numbers=dims, preferred_element_type=F32)
    return d(ah, bh) + (d(ah, bl) + d(al, bh))


def dot2(a, b, dims=NN):
    ah, al = split(a)
    b = b.astype(BF)
    d = functools.partial(lax.dot_general, dimension_numbers=dims, preferred_element_type=F32)
    return d(ah, b) + d(al, b)


def dot2r(a, b, dims=NN):
    bh, bl = split(b)
    a = a.astype(BF)
    d = functools.partial(lax.dot_general, dimension_numbers=dims, preferred_element_type=F32)
    return d(a, bh) + d(a, bl)


def lane_masks():
    lane = lax.broadcasted_iota(jnp.int32, (1, PAIR), 1)
    return lane < HEAD


def blocks_of(x, first):
    return jnp.concatenate([jnp.where(first, x, 0.0), jnp.where(first, 0.0, x)], axis=0)


def same_head():
    i = lax.broadcasted_iota(jnp.int32, (PAIR, PAIR), 0) // HEAD
    j = lax.broadcasted_iota(jnp.int32, (PAIR, PAIR), 1) // HEAD
    return (i == j).astype(F32).astype(BF)


def local_kernel(
    r_ref, k_ref, v_ref, d_ref, a_ref, off_ref, self_ref, g_ref, f_ref, bonus_ref, map_ref
):
    rows = r_ref.shape[0]
    first = lane_masks()
    ones = same_head()
    r, k, v = (x[...].astype(F32) for x in (r_ref, k_ref, v_ref))
    unit = k * lax.rsqrt(dot2(k * k, ones) + 1.0)
    log_decay = -DECAY_SCALE / (1.0 + jnp.exp(-(off_ref[...] + d_ref[...].astype(F32))))
    rate = 1.0 / (1.0 + jnp.exp(-a_ref[...].astype(F32)))
    b = unit * rate
    bonus_ref[...] = dot2(r * k * self_ref[...], ones) * v
    t_at = lax.broadcasted_iota(jnp.int32, (CHUNK, PAIR), 0)
    s_at = lax.broadcasted_iota(jnp.int32, (CHUNK, PAIR), 1) % HEAD
    strict, upto = s_at < t_at, s_at <= t_at
    eye = (s_at == t_at).astype(F32)
    tri = (
        lax.broadcasted_iota(jnp.int32, (CHUNK, CHUNK), 1)
        <= lax.broadcasted_iota(jnp.int32, (CHUNK, CHUNK), 0)
    ).astype(F32).astype(BF)
    moves, sums = None, None
    for c in range(rows // CHUNK):
        at = slice(c * CHUNK, (c + 1) * CHUNK)
        ld = log_decay[at]
        hi, lo = split(ld)
        lo2 = (ld - hi.astype(F32) - lo.astype(F32)).astype(BF)
        cum = (
            lax.dot_general(tri, hi, NN, preferred_element_type=F32)
            + lax.dot_general(tri, lo, NN, preferred_element_type=F32)
            + lax.dot_general(tri, lo2, NN, preferred_element_type=F32)
        )
        total = cum[CHUNK - 1 : CHUNK]
        inverse = jnp.exp(-cum)
        rest = jnp.exp(total - cum)
        kh = unit[at] * jnp.exp(cum - ld)
        rt = r[at] * jnp.exp(cum)
        vc = v[at]
        pairwise = dot3(
            jnp.concatenate([kh, rt], axis=0),
            jnp.concatenate([blocks_of(b[at] * inverse, first), blocks_of(k[at] * inverse, first)], axis=0),
            NT,
        )
        a_ub = jnp.where(strict, pairwise[:CHUNK, :PAIR], 0.0)
        a_uk = jnp.where(strict, pairwise[:CHUNK, PAIR:], 0.0)
        a_rb = jnp.where(upto, pairwise[CHUNK:, :PAIR], 0.0)
        a_rk = jnp.where(upto, pairwise[CHUNK:, PAIR:], 0.0)
        solve = eye
        size = 1
        while size < CHUNK:
            inside = ((t_at // size) % 2 == 1) & (s_at // size == t_at // size - 1)
            corner = jnp.where(inside, a_ub, 0.0)
            if size == 1:
                solve = eye - corner
            else:
                solve = solve - dot3(dot3(solve, blocks_of(corner, first)), blocks_of(solve, first))
            size *= 2
        w = dot2(jnp.concatenate([a_uk, a_rk], axis=0), blocks_of(vc, first))
        yx = dot3(
            solve, jnp.concatenate([blocks_of(kh, first), blocks_of(w[:CHUNK], first)], axis=1)
        )
        z = dot3(
            a_rb,
            jnp.concatenate(
                [blocks_of(yx[:, :PAIR], first), blocks_of(yx[:, PAIR:], first)], axis=1
            ),
        )
        q = rt - z[:, :PAIR]
        own = w[CHUNK:] - z[:, PAIR:]
        back = dot3(yx, b[at] * rest, TN)
        fresh = dot2r(vc, k[at] * rest, TN)

        def pick(m):
            return jnp.where(first, m[:HEAD], m[HEAD:])

        move = eye * jnp.exp(total) - pick(back[:PAIR])
        gain = pick(fresh) - pick(back[PAIR:])
        if c == 0:
            g_ref[at] = q.astype(g_ref.dtype)
            f_ref[at] = own
            moves, sums = move, gain
        else:
            gf = dot3(
                q,
                jnp.concatenate([blocks_of(moves, first), blocks_of(sums, first)], axis=0),
                NT,
            )
            g_ref[at] = gf[:, :PAIR].astype(g_ref.dtype)
            f_ref[at] = own + gf[:, PAIR:]
            both = dot3(jnp.concatenate([moves, sums], axis=0), blocks_of(move, first))
            moves, sums = both[:HEAD], both[HEAD:] + gain
    map_ref[0, :HEAD] = moves
    map_ref[0, HEAD:] = sums


def local_maps(r, k, v, d, a, off, self_weight):
    rows, width = r.shape
    pairs = width // PAIR
    block = pl.BlockSpec((rows, PAIR), lambda p: (0, p))
    vector = pl.BlockSpec((1, PAIR), lambda p: (0, p))
    return pl.pallas_call(
        local_kernel,
        grid=(pairs,),
        in_specs=[block] * 5 + [vector] * 2,
        out_specs=[block] * 3 + [pl.BlockSpec((1, PAIR, PAIR), lambda p: (p, 0, 0))],
        out_shape=[
            jax.ShapeDtypeStruct((rows, width), BF),
            jax.ShapeDtypeStruct((rows, width), F32),
            jax.ShapeDtypeStruct((rows, width), F32),
            jax.ShapeDtypeStruct((pairs, PAIR, PAIR), F32),
        ],
        cost_estimate=pl.CostEstimate(
            flops=30_000_000_000 // 3, bytes_accessed=8 * rows * width, transcendentals=0
        ),
        name="local_maps",
    )(r, k, v, d, a, off.reshape(1, -1), self_weight.reshape(1, -1))


def compose_kernel(before_ref, map_ref, out_ref, sent_ref):
    first = lane_masks()
    for p in range(map_ref.shape[0]):
        out = dot2r(before_ref[p], blocks_of(map_ref[p, :HEAD], first))
        out = jnp.concatenate([out[:HEAD], out[HEAD:] + map_ref[p, HEAD:]], axis=0)
        out_ref[p] = out
        sent_ref[p] = out.astype(BF)


def compose(before, current):
    return pl.pallas_call(
        compose_kernel,
        out_shape=[
            jax.ShapeDtypeStruct(current.shape, F32),
            jax.ShapeDtypeStruct(current.shape, BF),
        ],
        cost_estimate=pl.CostEstimate(flops=500_000_000, bytes_accessed=10 * current.size, transcendentals=0),
        name="compose_maps",
    )(before, current)


def readout_kernel(g_ref, f_ref, bonus_ref, gate_ref, s_ref, gain_ref, w_ref, out_ref, mixed):
    @pl.when(pl.program_id(0) == 0)
    def _():
        first = lane_masks()
        ones = same_head()
        for p in range(s_ref.shape[0]):
            at = slice(p * PAIR, (p + 1) * PAIR)
            state = s_ref[p].astype(F32)
            o = f_ref[:, at] + dot1(g_ref[:, at], blocks_of(state, first), NT)
            centred = o - dot2(o, ones) * (1.0 / HEAD)
            variance = dot2(centred * centred, ones) * (1.0 / HEAD)
            normed = centred * lax.rsqrt(variance + NORM_FLOOR) * gain_ref[:, at]
            mixed[:, at] = ((normed + bonus_ref[:, at]) * gate_ref[:, at].astype(F32)).astype(BF)

    out_ref[...] = jnp.dot(mixed[...], w_ref[...], preferred_element_type=F32).astype(BF)


def readout(g, f, bonus, gate, state, gain, w):
    rows, width = g.shape
    out_width = w.shape[1]
    tile = out_width // 4
    whole = pl.BlockSpec((rows, width), lambda n: (0, 0))
    return pl.pallas_call(
        readout_kernel,
        grid=(4,),
        in_specs=[whole] * 4
        + [
            pl.BlockSpec(state.shape, lambda n: (0, 0, 0)),
            pl.BlockSpec((1, width), lambda n: (0, 0)),
            pl.BlockSpec((width, tile), lambda n: (0, n)),
        ],
        out_specs=pl.BlockSpec((rows, tile), lambda n: (0, n)),
        out_shape=jax.ShapeDtypeStruct((rows, out_width), BF),
        scratch_shapes=[pltpu.VMEM((rows, width), BF)],
        cost_estimate=pl.CostEstimate(flops=3_000_000_000, bytes_accessed=4_000_000, transcendentals=0),
        name="readout",
    )(g, f, bonus, gate, state, gain.reshape(1, -1), w)


def shifted(x, axis, offset, wrap):
    n = lax.axis_size(axis)
    if wrap:
        pairs = [(i, (i + offset) % n) for i in range(n)]
    else:
        pairs = [(i, i + offset) for i in range(n) if 0 <= i + offset < n]
    return lax.ppermute(x, axis, pairs)


def flipped(x, axis, k):
    return lax.ppermute(x, axis, [(i, i ^ k) for i in range(lax.axis_size(axis))])


def mixer_part(r, k, v, d, a, gate, off, gain, self_weight, w):
    g, f, bonus, current = local_maps(r, k, v, d, a, off, self_weight)
    sent = current.astype(BF)
    step = 1
    while step < lax.axis_size("ep"):
        current, sent = compose(shifted(sent, "ep", step, False), current)
        step *= 2
    state = shifted(sent[:, HEAD:], "ep", 1, False)
    partial = readout(g, f, bonus, gate, state, gain, w)
    n_tp, me = lax.axis_size("tp"), lax.axis_index("tp")
    rows = partial.shape[0] // n_tp
    mine = lax.dynamic_slice_in_dim(partial, me * rows, rows, 0)
    received = [
        flipped(lax.dynamic_slice_in_dim(partial, (me ^ k) * rows, rows, 0), "tp", k)
        for k in range(1, n_tp)
    ]
    total = mine.astype(F32)
    for part in received:
        total = total + part.astype(F32)
    return total.astype(BF)


def gather_rows(x):
    chips = lax.axis_size("ep") // 2
    blocks, offsets = [x], [0]
    ahead, behind = x, x
    for s in range(1, (chips - 1) // 2 + 1):
        ahead, behind = shifted(ahead, "ep", 2, True), shifted(behind, "ep", -2, True)
        blocks += [ahead, behind]
        offsets += [s, -s]
    if chips % 2 == 0:
        half = x.shape[0] // 2
        blocks.append(
            jnp.concatenate(
                [shifted(ahead[:half], "ep", 2, True), shifted(behind[half:], "ep", -2, True)], axis=0
            )
        )
        offsets.append(chips // 2)
    return jnp.stack(blocks), offsets


def rounded(x):
    return lax.reduce_precision(x, 8, 7)


def expert_part(
    rows_in, index, weight, norm_gain, gate_w, up_w, down_w, common_gate, common_up, common_down
):
    row_count, width = rows_in.shape
    n_ep, n_tp = lax.axis_size("ep"), lax.axis_size("tp")
    me, tp_me = lax.axis_index("ep"), lax.axis_index("tp")
    slots = 3 * row_count * index.shape[1] // (2 * n_ep)
    wide = rows_in.astype(F32)
    normed = (
        wide * lax.rsqrt(jnp.mean(wide * wide, axis=-1, keepdims=True) + NORM_FLOOR) * norm_gain
    ).astype(BF)
    hit = index[:, :, None] == jnp.arange(n_ep, dtype=jnp.int32)
    named = jnp.any(hit, axis=1)
    tri = (jnp.arange(row_count)[None, :] < jnp.arange(row_count)[:, None]).astype(BF)
    rank = jnp.dot(tri, named.astype(BF), preferred_element_type=F32)
    rank = jnp.where(named, rank, 255.0)
    share = jnp.sum(jnp.where(hit, weight[:, :, None], 0.0), axis=1)
    top = rounded(share)
    middle = rounded(share - top)
    bottom = share - top - middle
    notes = jnp.concatenate([rank, top, middle, bottom], axis=1).astype(BF)
    notes = jnp.pad(notes, ((0, 0), (0, -notes.shape[1] % 128)))
    mine, offsets = gather_rows(jnp.concatenate([normed, notes], axis=1))
    count = len(offsets)
    blocks = jnp.concatenate([mine, flipped(mine, "ep", 1)], axis=0)
    own_notes = blocks[:, :, width : width + 4 * n_ep].astype(F32).reshape(2 * count, row_count, 4, n_ep)
    own_notes = jnp.sum(jnp.where(jnp.arange(n_ep) == me, own_notes, 0.0), axis=3)
    slot = own_notes[:, :, 0].astype(jnp.int32)
    share_here = own_notes[:, :, 1] + own_notes[:, :, 2] + own_notes[:, :, 3]
    choose = (slot[:, None, :] == jnp.arange(slots, dtype=jnp.int32)[None, :, None]).astype(BF)
    chosen = jnp.einsum("bsr,brd->bsd", choose, blocks[:, :, :width], preferred_element_type=F32)
    chosen = chosen.astype(BF).reshape(2 * count * slots, width)

    def activate(x, gate_part, up_part):
        pre_gate = jnp.einsum("fd,rd->rf", gate_part, x, preferred_element_type=F32)
        pre_up = jnp.einsum("fd,rd->rf", up_part, x, preferred_element_type=F32)
        return (jax.nn.silu(pre_gate) * pre_up).astype(BF)

    hidden = jnp.concatenate(
        [activate(chosen, gate_w[0], up_w[0]), activate(normed, common_gate, common_up)], axis=0
    )
    units = hidden.shape[1]
    pieces = [hidden] + [flipped(hidden, "tp", k) for k in range(1, n_tp)]
    hidden = jnp.concatenate(pieces, axis=1)

    def reordered(w):
        return jnp.concatenate(
            [lax.dynamic_slice_in_dim(w, (tp_me ^ k) * units, units, 0) for k in range(n_tp)], axis=0
        )

    routed = 2 * count * slots
    copies = jnp.dot(hidden[:routed], reordered(down_w[0]), preferred_element_type=F32).astype(BF)
    shared = jnp.dot(hidden[routed:], reordered(common_down), preferred_element_type=F32)
    spread = jnp.einsum(
        "bsr,bsd->brd", choose, copies.reshape(2 * count, slots, -1), preferred_element_type=F32
    )
    spread = spread * share_here[:, :, None]
    there = flipped(spread[count:].astype(BF), "ep", 1)
    both = spread[:count] + there.astype(F32)
    total = both[0] + shared
    for i, offset in enumerate(offsets):
        if i:
            total = total + shifted(both[i].astype(BF), "ep", -2 * offset, True).astype(F32)
    return total.astype(BF)


def on_device(*args):
    return mixer_part(*args[:10]), expert_part(*args[10:])


def solution(mesh):
    in_specs = (
        (P("ep", "tp"),) * 6
        + (P("tp"),) * 3
        + (P("tp", None),)
        + (P("ep", None),) * 3
        + (P(),)
        + (P("ep", "tp", None),) * 2
        + (P("ep", None, "tp"),)
        + (P("tp", None),) * 2
        + (P(None, "tp"),)
    )
    out_specs = (P(("ep", "tp"), None), P("ep", "tp"))
    return jax.shard_map(
        on_device, mesh=mesh, in_specs=in_specs, out_specs=out_specs, check_vma=False
    )
```

```python
import functools

import jax
import jax.numpy as jnp
from jax import lax
from jax.experimental import pallas as pl
from jax.experimental.pallas import tpu as pltpu
from jax.sharding import PartitionSpec as P


GRANT = 20 * 1024 * 1024
HEAD = 64
PAIR = 2 * HEAD
CHUNK = 64
NORM_FLOOR = 1.0
DECAY_SCALE = 0.6065306597126334
BF = jnp.bfloat16
F32 = jnp.float32
NN = (((1,), (0,)), ((), ()))
NT = (((1,), (1,)), ((), ()))
TN = (((0,), (0,)), ((), ()))


def dot1(a, b, dims=NN):
    return lax.dot_general(a.astype(BF), b.astype(BF), dims, preferred_element_type=F32)


def split(x):
    hi = x.astype(BF)
    return hi, (x - hi.astype(F32)).astype(BF)


def joined(parts, dims, product):
    (ah, al), (bh, bl) = parts
    keep_a, keep_b = 1 - dims[0][0][0], 1 - dims[0][1][0]
    m, n = ah.shape[keep_a], bh.shape[keep_b]
    out = product(jnp.concatenate([ah, al], axis=keep_a), jnp.concatenate([bh, bl], axis=keep_b))
    return out[:m, :n] + (out[:m, n:] + out[m:, :n])


def dot3(a, b, dims=NN):
    a = a if isinstance(a, tuple) else split(a)
    b = b if isinstance(b, tuple) else split(b)
    product = functools.partial(lax.dot_general, dimension_numbers=dims, preferred_element_type=F32)
    return joined((a, b), dims, product)


def dot2(a, b, dims=NN):
    ah, al = split(a)
    keep = 1 - dims[0][0][0]
    m = ah.shape[keep]
    both = jnp.concatenate([ah, al], axis=keep)
    out = lax.dot_general(both, b.astype(BF), dims, preferred_element_type=F32)
    return out[:m] + out[m:]


def dot2r(a, b, dims=NN):
    bh, bl = b if isinstance(b, tuple) else split(b)
    keep = 1 - dims[0][1][0]
    n = bh.shape[keep]
    both = jnp.concatenate([bh, bl], axis=keep)
    out = lax.dot_general(a.astype(BF), both, dims, preferred_element_type=F32)
    return out[:, :n] + out[:, n:]


def lane_masks():
    lane = lax.broadcasted_iota(jnp.int32, (1, PAIR), 1)
    return lane < HEAD


def blocks_of(x, first):
    return jnp.concatenate([jnp.where(first, x, 0.0), jnp.where(first, 0.0, x)], axis=0)


def split_blocks(x, first):
    one = first.astype(F32).astype(BF)
    return tuple(jnp.concatenate([h * one, h * (1 - one)], axis=0) for h in split(x))


def beside(a, b, axis):
    return tuple(jnp.concatenate([x, y], axis=axis) for x, y in zip(a, b, strict=True))


def same_head():
    i = lax.broadcasted_iota(jnp.int32, (PAIR, PAIR), 0) // HEAD
    j = lax.broadcasted_iota(jnp.int32, (PAIR, PAIR), 1) // HEAD
    return (i == j).astype(F32).astype(BF)


def local_kernel(
    pairs,
    r_ref,
    k_ref,
    v_ref,
    d_ref,
    a_ref,
    off_ref,
    self_ref,
    parts_ref,
    sent_ref,
):
    rows, width = r_ref.shape[0], parts_ref.shape[1] // 3
    first = lane_masks()
    ones = same_head()
    t_at = lax.broadcasted_iota(jnp.int32, (CHUNK, PAIR), 0)
    s_at = lax.broadcasted_iota(jnp.int32, (CHUNK, PAIR), 1) % HEAD
    strict, upto = s_at < t_at, s_at <= t_at
    eye = (s_at == t_at).astype(F32)
    tri = (
        lax.broadcasted_iota(jnp.int32, (CHUNK, CHUNK), 1)
        <= lax.broadcasted_iota(jnp.int32, (CHUNK, CHUNK), 0)
    ).astype(F32).astype(BF)
    chunks = rows // CHUNK
    rts, khs, rights, lefts, vs, totals = [], [], [], [], [], []
    for n, pair in enumerate(pairs):
        lanes = slice(pair * PAIR, (pair + 1) * PAIR)
        r, k, v = (x[:, lanes].astype(F32) for x in (r_ref, k_ref, v_ref))
        unit = k * lax.rsqrt(dot2(k * k, ones) + 1.0)
        log_decay = -DECAY_SCALE / (
            1.0 + jnp.exp(-(off_ref[:, lanes] + d_ref[:, lanes].astype(F32)))
        )
        b = unit / (1.0 + jnp.exp(-a_ref[:, lanes].astype(F32)))
        to = slice(2 * width + n * PAIR, 2 * width + (n + 1) * PAIR)
        parts_ref[:, to] = dot2(r * k * self_ref[:, lanes], ones) * v
        hi, lo = split(log_decay)
        lo2 = (log_decay - hi.astype(F32) - lo.astype(F32)).astype(BF)
        for c in range(chunks):
            at = slice(c * CHUNK, (c + 1) * CHUNK)
            three = jnp.concatenate([hi[at], lo[at], lo2[at]], axis=1)
            out = lax.dot_general(tri, three, NN, preferred_element_type=F32)
            cum = out[:, :PAIR] + out[:, PAIR : 2 * PAIR] + out[:, 2 * PAIR :]
            total = cum[CHUNK - 1 : CHUNK]
            inverse, rest = jnp.exp(-cum), jnp.exp(total - cum)
            khs.append(unit[at] * jnp.exp(cum - log_decay[at]))
            rts.append(r[at] * jnp.exp(cum))
            vs.append(v[at])
            rights.append(
                beside(split_blocks(b[at] * inverse, first), split_blocks(k[at] * inverse, first), 0)
            )
            lefts.append((split(b[at] * rest), split(k[at] * rest)))
            totals.append(total)
    pairwise = [
        dot3(jnp.concatenate([kh, rt], axis=0), right, NT) for kh, rt, right in zip(khs, rts, rights)
    ]
    a_ubs = [jnp.where(strict, p[:CHUNK, :PAIR], 0.0) for p in pairwise]
    a_rbs = [jnp.where(upto, p[CHUNK:, :PAIR], 0.0) for p in pairwise]
    ws = []
    for v, p in zip(vs, pairwise):
        left = jnp.concatenate(
            [jnp.where(strict, p[:CHUNK, PAIR:], 0.0), jnp.where(upto, p[CHUNK:, PAIR:], 0.0)], axis=0
        )
        ws.append(dot2(left, blocks_of(v, first)))

    def corner_of(size):
        inside = ((t_at // size) % 2 == 1) & (s_at // size == t_at // size - 1)
        return [jnp.where(inside, a_ub, 0.0) for a_ub in a_ubs]

    solves = [eye - corner for corner in corner_of(1)]
    size = 2
    while size < CHUNK:
        halfway = [
            dot3(solve, split_blocks(corner, first)) for solve, corner in zip(solves, corner_of(size))
        ]
        solves = [
            solve - dot3(half, split_blocks(solve, first)) for half, solve in zip(halfway, solves)
        ]
        size *= 2
    yxs = [
        dot3(solve, beside(split_blocks(kh, first), split_blocks(w[:CHUNK], first), 1))
        for solve, kh, w in zip(solves, khs, ws)
    ]
    zs = [
        dot3(a_rb, beside(split_blocks(yx[:, :PAIR], first), split_blocks(yx[:, PAIR:], first), 1))
        for a_rb, yx in zip(a_rbs, yxs)
    ]

    def pick(m):
        return jnp.where(first, m[:HEAD], m[HEAD:])

    moves, gains = [], []
    for total, yx, v, (b_rest, k_rest) in zip(totals, yxs, vs, lefts):
        back = dot3(yx, b_rest, TN)
        fresh = dot2r(v, k_rest, TN)
        moves.append(eye * jnp.exp(total) - pick(back[:PAIR]))
        gains.append(pick(fresh) - pick(back[PAIR:]))
    current = [(moves[n * chunks], gains[n * chunks]) for n in range(len(pairs))]
    befores = {}
    for c in range(1, chunks):
        for n, (move, gain) in enumerate(current):
            u = n * chunks + c
            befores[u] = beside(split_blocks(move, first), split_blocks(gain, first), 0)
            both = dot3(jnp.concatenate([move, gain], axis=0), split_blocks(moves[u], first))
            current[n] = (both[:HEAD], both[HEAD:] + gains[u])
    for c in range(chunks):
        for n in range(len(pairs)):
            u = n * chunks + c
            at, to = slice(c * CHUNK, (c + 1) * CHUNK), slice(n * PAIR, (n + 1) * PAIR)
            q = rts[u] - zs[u][:, :PAIR]
            own = ws[u][CHUNK:] - zs[u][:, PAIR:]
            if c:
                gf = dot3(q, befores[u], NT)
                q, own = gf[:, :PAIR], own + gf[:, PAIR:]
            parts_ref[at, to] = q
            parts_ref[at, slice(width + n * PAIR, width + (n + 1) * PAIR)] = own
    for n, (move, gain) in enumerate(current):
        out = jnp.concatenate([move, gain], axis=0)
        sent_ref[n] = out.astype(BF)


def in_vmem(count):
    return [pl.BlockSpec(memory_space=pltpu.VMEM)] * count


def local_maps(r, k, v, d, a, off, self_weight, pairs):
    rows, count = r.shape[0], len(pairs)
    return pl.pallas_call(
        functools.partial(local_kernel, pairs),
        in_specs=in_vmem(7),
        out_specs=in_vmem(2),
        out_shape=[
            jax.ShapeDtypeStruct((rows, 3 * count * PAIR), F32),
            jax.ShapeDtypeStruct((count, PAIR, PAIR), BF),
        ],
        cost_estimate=pl.CostEstimate(
            flops=6_000_000_000 * count, bytes_accessed=20 * rows * PAIR * count, transcendentals=0
        ),
        compiler_params=pltpu.CompilerParams(vmem_limit_bytes=GRANT),
        name="local_maps",
    )(r, k, v, d, a, off.reshape(1, -1), self_weight.reshape(1, -1))


def chip_kernel(place_ref, own_ref, other_ref, out_ref):
    first = lane_masks()
    core = place_ref[1]
    for p in range(out_ref.shape[0]):
        own, other = own_ref[p].astype(F32), other_ref[p].astype(F32)
        early = jnp.where(core == 0, own, other)
        late = jnp.where(core == 0, other, own)
        out = dot2(early, blocks_of(late[:HEAD], first))
        out_ref[p, :HEAD] = out[:HEAD].astype(BF)
        out_ref[p, HEAD:] = (out[HEAD:] + late[HEAD:]).astype(BF)


def chip_maps(place, own, other):
    return pl.pallas_call(
        chip_kernel,
        in_specs=[pl.BlockSpec(memory_space=pltpu.SMEM)] + in_vmem(2),
        out_specs=pl.BlockSpec(memory_space=pltpu.VMEM),
        out_shape=jax.ShapeDtypeStruct(own.shape, BF),
        cost_estimate=pl.CostEstimate(flops=1_000_000_000, bytes_accessed=10 * own.size, transcendentals=0),
        compiler_params=pltpu.CompilerParams(vmem_limit_bytes=GRANT),
        name="chip_maps",
    )(place, own, other)


def readout_kernel(each, place_ref, other_ref, gate_ref, gain_ref, w_ref, *refs):
    befores, refs = refs[: each[2]], refs[each[2] :]
    *parts, mixed = refs
    outs = parts[each[1] :]
    first = lane_masks()
    ones = same_head()
    core, tp = place_ref[1], place_ref[2]
    pairs = other_ref.shape[0]
    states = [befores[-1][p, HEAD:].astype(F32) for p in range(pairs)] if befores else []
    for m in befores[-2::-1]:
        states = [
            dot2(state, blocks_of(m[p, :HEAD].astype(F32), first)) + m[p, HEAD:].astype(F32)
            for p, state in enumerate(states)
        ]
    late = [
        dot2(state, blocks_of(other_ref[p, :HEAD].astype(F32), first))
        + other_ref[p, HEAD:].astype(F32)
        for p, state in enumerate(states)
    ]
    states = [jnp.where(core == 1, x, y) for x, y in zip(late, states)]
    for p in range(pairs):
        call, n = divmod(p, each[0])
        at = slice(p * PAIR, (p + 1) * PAIR)
        g, f, bonus = (
            parts[call][:, (i * each[0] + n) * PAIR : (i * each[0] + n + 1) * PAIR] for i in range(3)
        )
        o = f + dot1(g, blocks_of(states[p], first), NT)
        centred = o - dot2(o, ones) * (1.0 / HEAD)
        variance = dot2(centred * centred, ones) * (1.0 / HEAD)
        normed = centred * lax.rsqrt(variance + NORM_FLOOR) * gain_ref[:, at]
        mixed[:, at] = ((normed + bonus) * gate_ref[:, at].astype(F32)).astype(BF)
    rows = outs[0].shape[0]
    order = jnp.concatenate(
        [mixed[pl.ds(pl.multiple_of((tp ^ k) * rows, rows), rows), :] for k in range(len(outs))], axis=0
    )
    width = w_ref.shape[1]
    tile = width // 4
    for n in range(0, width, tile):
        part = jnp.dot(order, w_ref[:, n : n + tile], preferred_element_type=F32).astype(BF)
        for k, out_ref in enumerate(outs):
            out_ref[:, n : n + tile] = part[k * rows : (k + 1) * rows]


def readout(place, befores, other, gate, gain, w, parts, each, n_tp):
    rows, width = gate.shape
    flat = parts
    shape = jax.ShapeDtypeStruct((rows // n_tp, w.shape[1]), BF)
    return pl.pallas_call(
        functools.partial(readout_kernel, (each, len(flat), len(befores))),
        in_specs=[pl.BlockSpec(memory_space=pltpu.SMEM)] + in_vmem(4 + len(befores) + len(flat)),
        out_specs=in_vmem(n_tp),
        out_shape=[shape] * n_tp,
        scratch_shapes=[pltpu.VMEM((rows, width), BF)],
        cost_estimate=pl.CostEstimate(flops=6_000_000_000, bytes_accessed=4_000_000, transcendentals=0),
        compiler_params=pltpu.CompilerParams(vmem_limit_bytes=GRANT),
        name="readout",
    )(place, other, gate, gain.reshape(1, -1), w, *befores, *flat)


def stack_kernel(*refs):
    at, out_ref = 0, refs[-1]
    for x_ref in refs[:-1]:
        out_ref[at : at + x_ref.shape[0]] = x_ref[...]
        at += x_ref.shape[0]


def stacked(xs):
    rows = sum(x.shape[0] for x in xs)
    return pl.pallas_call(
        stack_kernel,
        in_specs=in_vmem(len(xs)),
        out_specs=pl.BlockSpec(memory_space=pltpu.VMEM),
        out_shape=jax.ShapeDtypeStruct((rows, *xs[0].shape[1:]), xs[0].dtype),
        cost_estimate=pl.CostEstimate(flops=1_000_000, bytes_accessed=1_000_000, transcendentals=0),
        compiler_params=pltpu.CompilerParams(vmem_limit_bytes=GRANT),
        name="stacked",
    )(*xs)


def shifted(x, axis, offset, wrap):
    n = lax.axis_size(axis)
    if wrap:
        pairs = [(i, (i + offset) % n) for i in range(n)]
    else:
        pairs = [(i, i + offset) for i in range(n) if 0 <= i + offset < n]
    return lax.ppermute(x, axis, pairs)


def flipped(x, axis, k):
    return lax.ppermute(x, axis, [(i, i ^ k) for i in range(lax.axis_size(axis))])


PAIRS_EACH = 2


def mixer_part(place, r, k, v, d, a, gate, off, gain, self_weight, w):
    pairs = r.shape[1] // PAIR
    n_tp = lax.axis_size("tp")
    chips = lax.axis_size("ep") // 2
    each = min(PAIRS_EACH, pairs)
    local = [local_maps(r, k, v, d, a, off, self_weight, range(p, p + each)) for p in range(0, pairs, each)]
    parts = [x[0] for x in local]
    own = local[0][1] if len(local) == 1 else stacked([x[1] for x in local])
    other = flipped(own, "ep", 1)
    chip = chip_maps(place, own, other)
    before = [shifted(chip, "ep", 2 * s, False) for s in range(1, chips)]
    mine, *others = readout(place, before, other, gate, gain, w, parts, each, n_tp)
    total = mine.astype(F32)
    for k, part in enumerate(others, 1):
        total = total + flipped(part, "tp", k).astype(F32)
    return total.astype(BF)


def prepare_kernel(n_ep, x_ref, index_ref, weight_ref, gain_ref, out_ref, share_ref):
    rows, width = x_ref.shape
    wide = x_ref[...].astype(F32)
    scale = lax.rsqrt(jnp.sum(wide * wide, axis=1, keepdims=True) * (1.0 / width) + NORM_FLOOR)
    out_ref[:, :width] = (wide * scale * gain_ref[...]).astype(BF)
    noted = out_ref.shape[1] - width
    lane = lax.broadcasted_iota(jnp.int32, (rows, noted), 1)
    expert = jnp.where(lane < 4 * n_ep, lane % n_ep, -1).astype(F32)
    named = jnp.zeros((rows, noted), F32)
    share = jnp.zeros((rows, noted), F32)
    tops = index_ref.shape[0]
    turn = (
        lax.broadcasted_iota(jnp.int32, (rows, rows), 0)
        == lax.broadcasted_iota(jnp.int32, (rows, rows), 1)
    ).astype(F32).astype(BF)
    high, low = split(weight_ref[...])
    lower = (weight_ref[...] - high.astype(F32) - low.astype(F32)).astype(BF)
    columns = [
        lax.dot_general(turn, x, NT, preferred_element_type=F32)
        for x in (index_ref[...].astype(F32).astype(BF), high, low, lower)
    ]
    weights = columns[1] + columns[2] + columns[3]
    for t in range(tops):
        hit = columns[0][:, t : t + 1] == expert
        named = named + jnp.where(hit, 1.0, 0.0)
        share = share + jnp.where(hit, weights[:, t : t + 1], 0.0)
    above = (
        lax.broadcasted_iota(jnp.int32, (rows, rows), 1)
        < lax.broadcasted_iota(jnp.int32, (rows, rows), 0)
    ).astype(F32)
    rank = jnp.where(named > 0.0, dot1(above, named), 255.0)
    top = share.astype(BF).astype(F32)
    middle = (share - top).astype(BF).astype(F32)
    part = lane // n_ep
    notes = jnp.where(
        part == 0,
        rank,
        jnp.where(part == 1, top, jnp.where(part == 2, middle, share - top - middle)),
    ).astype(BF)
    out_ref[:, width:] = notes
    piece = share_ref.shape[0]
    share_ref[...] = out_ref[pl.ds(pl.multiple_of(lax.axis_index("tp") * piece, piece), piece), :]


def prepare(rows_in, index, weight, gain):
    rows, width = rows_in.shape
    n_ep = lax.axis_size("ep")
    noted = -(-4 * n_ep // 128) * 128
    return pl.pallas_call(
        functools.partial(prepare_kernel, n_ep),
        in_specs=in_vmem(4),
        out_specs=in_vmem(2),
        out_shape=[
            jax.ShapeDtypeStruct((rows, width + noted), BF),
            jax.ShapeDtypeStruct((rows // lax.axis_size("tp"), width + noted), BF),
        ],
        cost_estimate=pl.CostEstimate(flops=1_000_000_000, bytes_accessed=2_000_000, transcendentals=0),
        name="prepare",
    )(rows_in, index.T, weight.T, gain.reshape(1, -1))


def slots_of(notes, me, slots):
    want = (lax.broadcasted_iota(jnp.int32, (8, notes.shape[1]), 1) == me).astype(F32).astype(BF)
    rank = lax.dot_general(want, notes, NT, preferred_element_type=F32)[:1]
    slot = lax.broadcasted_iota(jnp.int32, (slots, notes.shape[0]), 0).astype(F32)
    return (slot == rank).astype(F32).astype(BF)


def hidden_kernel(parts, slots, shared, count, place_ref, *refs):
    arrays, refs = refs[:count], refs[count:]
    weights, outs = refs[: 2 + 2 * shared], refs[2 + 2 * shared :]
    width = weights[0].shape[1]
    me = place_ref[0]

    def activate(x, gate_ref, up_ref):
        gate = lax.dot_general(x, gate_ref[...], NT, preferred_element_type=F32)
        up = lax.dot_general(x, up_ref[...], NT, preferred_element_type=F32)
        return (gate / (1.0 + jnp.exp(-gate)) * up).astype(BF)

    hidden = activate(jnp.concatenate([x[:, :width] for x in arrays], axis=0), *weights[:2])
    all_notes = jnp.concatenate([x[:, width:] for x in arrays], axis=0)
    for part, places in enumerate(parts):
        out_ref, notes_ref = outs[2 * part : 2 * part + 2]
        for n, block in enumerate(places):
            notes = jnp.concatenate([all_notes[at : at + size] for at, size in block], axis=0)
            units = jnp.concatenate([hidden[at : at + size] for at, size in block], axis=0)
            notes_ref[n] = notes
            choose = slots_of(notes, me, slots)
            out_ref[n * slots : (n + 1) * slots] = jnp.dot(
                choose, units, preferred_element_type=F32
            ).astype(BF)
    if shared:
        out_ref = outs[0]
        out_ref[len(parts[0]) * slots :] = activate(arrays[0][:, :width], *weights[2:])


def hidden_units(place, arrays, parts, slots, weights, shared):
    columns = arrays[0].shape[1]
    units, width = weights[0].shape
    rows = sum(size for _, size in parts[0][0])
    out_shape = []
    for places in parts:
        out_shape += [
            jax.ShapeDtypeStruct((len(places) * slots + (rows if shared else 0), units), BF),
            jax.ShapeDtypeStruct((len(places), rows, columns - width), BF),
        ]
    out = pl.pallas_call(
        functools.partial(hidden_kernel, parts, slots, shared, len(arrays)),
        in_specs=[pl.BlockSpec(memory_space=pltpu.SMEM)] + in_vmem(len(arrays) + len(weights)),
        out_specs=in_vmem(len(out_shape)),
        out_shape=out_shape,
        cost_estimate=pl.CostEstimate(flops=3_000_000_000, bytes_accessed=4_000_000, transcendentals=0),
        compiler_params=pltpu.CompilerParams(vmem_limit_bytes=GRANT),
        name="hidden_units",
    )(place, *arrays, *weights)
    return list(zip(out[::2], out[1::2]))


def outcome_kernel(slots, shared, turned, n_tp, n_ep, me_ref, *refs):
    hidden, notes_ref, refs = refs[:n_tp], refs[n_tp], refs[n_tp + 1 :]
    downs, outs = refs[: 1 + shared], refs[1 + shared :]
    mines, other_ref, ordered = outs[:-2], outs[-2], outs[-1]
    me, tp = me_ref[0], me_ref[2]
    units = hidden[0].shape[1]
    count, rows, noted = notes_ref.shape

    def product(lo, hi, down):
        out = None
        for k in range(n_tp):
            w = down[pl.ds(pl.multiple_of((tp ^ k) * units, units), units), :]
            part = jnp.dot(hidden[k][lo:hi], w, preferred_element_type=F32)
            out = part if out is None else out + part
        return out

    copies = product(0, count * slots, downs[0]).astype(BF)
    lane = lax.broadcasted_iota(jnp.int32, (rows, noted), 1)
    mark = (lane % n_ep == me) & (lane >= n_ep) & (lane < 4 * n_ep)
    extra = product(count * slots, hidden[0].shape[0], downs[1]) if shared else None
    for n in range(count):
        notes = notes_ref[n]
        choose = slots_of(notes, me, slots)
        share = jnp.sum(jnp.where(mark, notes.astype(F32), 0.0), axis=1, keepdims=True)
        spread = lax.dot_general(
            choose, copies[n * slots : (n + 1) * slots], TN, preferred_element_type=F32
        )
        spread = spread * share
        if n == 0 and shared:
            spread = spread + extra
        if turned:
            piece = rows // n_tp
            to = mines[n] if n < len(mines) else ordered
            for k in range(n_tp):
                at = pl.ds(pl.multiple_of((tp ^ k) * piece, piece), piece)
                to[at, :] = spread[k * piece : (k + 1) * piece]
            if n >= len(mines):
                other_ref[n - len(mines)] = ordered[...].astype(BF)
        elif n < len(mines):
            mines[n][...] = spread
        else:
            other_ref[n - len(mines)] = spread.astype(BF)


def outcomes(me, hidden, notes, slots, downs, turned):
    out_width = downs[0].shape[1]
    count, rows, _ = notes.shape
    half = count // 2
    return pl.pallas_call(
        functools.partial(
            outcome_kernel, slots, len(downs) - 1, turned, len(hidden), lax.axis_size("ep")
        ),
        in_specs=[pl.BlockSpec(memory_space=pltpu.SMEM)] + in_vmem(len(hidden) + 1 + len(downs)),
        out_specs=in_vmem(half + 1),
        out_shape=[jax.ShapeDtypeStruct((rows, out_width), F32)] * half
        + [jax.ShapeDtypeStruct((half, rows, out_width), BF)],
        scratch_shapes=[pltpu.VMEM((rows, out_width), F32)],
        cost_estimate=pl.CostEstimate(flops=3_000_000_000, bytes_accessed=3_000_000, transcendentals=0),
        compiler_params=pltpu.CompilerParams(vmem_limit_bytes=GRANT),
        name="outcomes",
    )(me, *hidden, notes, *downs)


def expert_part(
    place,
    rows_in,
    index,
    weight,
    norm_gain,
    gate_w,
    up_w,
    down_w,
    common_gate,
    common_up,
    common_down,
):
    n_ep, n_tp = lax.axis_size("ep"), lax.axis_size("tp")
    chips = n_ep // 2
    slots = 3 * rows_in.shape[0] * index.shape[1] // (2 * n_ep)
    slots = -(-slots // 16) * 16
    whole, own = prepare(rows_in, index, weight, norm_gain)
    piece = own.shape[0]
    offsets = list(range(1, chips))
    came = [shifted(own, "ep", 2 * s, True) for s in offsets]
    arrays, places, base = [], {}, 0
    for batch in (offsets,):
        if not batch:
            continue
        part = [came[s - 1] for s in batch]
        share = part[0] if len(part) == 1 else stacked(part)
        shares = [share] + [flipped(share, "tp", k) for k in range(1, n_tp)]
        swapped = [flipped(x, "ep", 1) for x in shares]
        for c, group in enumerate((shares, swapped)):
            for i, s in enumerate(batch):
                places[c, s] = [(base + k * share.shape[0] + i * piece, piece) for k in range(n_tp)]
            base += n_tp * share.shape[0]
            arrays += group
    batches = [[s for s in offsets if 2 * s == chips], [s for s in offsets if 2 * s != chips]]
    batches = [batch for batch in batches if batch]
    far = [[places[c, s] for c in range(2) for s in batch] for batch in batches]
    rows = whole.shape[0]
    near = [[[(0, rows)], [(rows, rows)]]]
    other_rows = flipped(whole, "ep", 1)
    weights = [gate_w[0], up_w[0]]
    (first,) = hidden_units(place, [whole, other_rows], near, slots, weights + [common_gate, common_up], True)
    rest = hidden_units(place, arrays, far, slots, weights, False)
    total = None
    for g, ((hidden, notes), sent) in enumerate(zip([first, *rest], [[0], *batches], strict=True)):
        hidden = [hidden] + [flipped(hidden, "tp", k) for k in range(1, n_tp)]
        downs = [down_w[0]] + ([common_down] if g == 0 else [])
        *mines, other = outcomes(place, hidden, notes, slots, downs, g > 0)
        there = flipped(other, "ep", 1)
        for i, (mine, offset) in enumerate(zip(mines, sent, strict=True)):
            both = mine + there[i].astype(F32)
            if offset:
                both = shifted(both.astype(BF), "ep", -2 * offset, True).astype(F32)
            total = both if total is None else total + both
    return total.astype(BF)


def on_device(*args):
    ep, tp = lax.axis_index("ep"), lax.axis_index("tp")
    place = jnp.stack([ep, ep % 2, tp]).astype(jnp.int32)
    return mixer_part(place, *args[:10]), expert_part(place, *args[10:])


def solution(mesh):
    in_specs = (
        (P("ep", "tp"),) * 6
        + (P("tp"),) * 3
        + (P("tp", None),)
        + (P("ep", None),) * 3
        + (P(),)
        + (P("ep", "tp", None),) * 2
        + (P("ep", None, "tp"),)
        + (P("tp", None),) * 2
        + (P(None, "tp"),)
    )
    out_specs = (P(("ep", "tp"), None), P("ep", "tp"))
    return jax.shard_map(
        on_device, mesh=mesh, in_specs=in_specs, out_specs=out_specs, check_vma=False
    )
```
